32 devices in a mesh: ep: 8 (over z, y), tp: 4 (over x, core).
Axes of the slice: x: 2, y: 2, z: 4, core: 2. Of those that a mesh axis runs over, the one named last changes fastest.
Arguments:
- value_in: bfloat16 [4096, 1024], P('ep', 'tp'), may hold values from -6 to 6
- gate_in: bfloat16 [4096, 1024], P('ep', 'tp'), may hold values from -6 to 6
- outer_gate: bfloat16 [4096, 1024], P('ep', 'tp'), may hold values from -6 to 6
- conv_weight: bfloat16 [3, 1024], P(None, 'tp'), may hold values from -3.5 to 3.5
- out_weight: bfloat16 [1024, 2048], P('tp'), may hold values from -0.1875 to 0.1875
- moe_tokens: bfloat16 [4096, 2048], P(('ep', 'tp')), may hold values from -6 to 6
- norm_gain: bfloat16 [2048], replicated, may hold values from 0.099609375 to 1.8984375
- routes: int32 [4096, 2], P(('ep', 'tp')), may hold values from 0 to 7, all different within a row; in each aligned block of 128 rows (0 to 127, 128 to 255, ...) at most 48 rows name the same one
- route_weight: float32 [4096, 2], P(('ep', 'tp')), may hold values from 0.1 to 1
- expert_gate: bfloat16 [8, 2048, 6144], P('ep', None, 'tp'), may hold values from -0.125 to 0.125
- expert_up: bfloat16 [8, 2048, 6144], P('ep', None, 'tp'), may hold values from -0.125 to 0.125
- expert_down: bfloat16 [8, 6144, 2048], P('ep', 'tp'), may hold values from -0.078125 to 0.078125
Outputs:
- mixer_out: bfloat16 [4096, 2048], P(('ep', 'tp'))
- moe_out: bfloat16 [4096, 2048], P(('ep', 'tp'))
The draws below stay inside these ranges and needn't reach their ends.
Inputs may be any that keep to these rules, and one draw needn't show every extreme that they name: `routes`: each row names 2 different experts. Among the rows of one device no expert is named by more than 48 rows, a bound that some blocks reach.
All inputs are finite; a program needn't handle non-finite values.
Results may differ from the reference program's by a relative error of at most 0.012.
Values may be sent and summed in bfloat16 or wider, within the bound.
A program may use at most 128 MiB of HBM per device.

```python
import math
import jax
import jax.numpy as jnp
import numpy as np
from jax import lax

D = 2048
CW = 1024
FFE = 6144
TOP = 2
TOK_DEV = 128
EXPERTS = 8
CAP = 48
TOKENS_A = 4096
TOKENS_B = 4096
N_TP = 4


def levels(own_key, dims, cuts, smallest, largest):
    level = 1.0
    for axis_at, blocks in cuts:
        heights = jax.random.uniform(jax.random.fold_in(jax.random.fold_in(own_key, 6), axis_at), (blocks,), jnp.float32, smallest / len(cuts), largest / len(cuts))
        level = level * jnp.repeat(jnp.exp(heights), dims[axis_at] // blocks).reshape((-1,) + (1,) * (len(dims) - 1 - axis_at))
    return level


def shared_out(stream_key, own, number, rows, amount, top, most, lean):
    order = jax.random.permutation(stream_key, amount)
    packed, usual = load_shares(amount, rows * top, most, lean, True), load_shares(amount, rows * top, most, lean, False)
    places = jnp.arange(amount)

    def named(tallies, rotation):
        used = int((tallies > 0).sum())
        fixed = max(1, used // 4)
        moved = fixed + (places - fixed + rotation * (used - fixed)) % max(1, amount - fixed)
        return jnp.zeros((amount,), jnp.int32).at[order[jnp.where(places < fixed, places, moved)]].set(jnp.asarray(tallies, jnp.int32))

    tallies = jnp.where(number % 4 == 0, named(packed, number // 4), named(usual, number - number // 4 - 1))
    mixed = jax.random.permutation(jax.random.fold_in(own, 3), amount)
    donor, sink = mixed[0:amount // 2 * 2:2], mixed[1:amount // 2 * 2:2]
    margin = jnp.minimum(tallies[donor] - 1, most - tallies[sink]) // 2
    margin = jnp.where((donor == order[0]) | (sink == order[0]) | (tallies[sink] == 0), 0, jnp.maximum(margin, 0))
    moved = jax.random.randint(jax.random.fold_in(own, 4), (amount // 2,), 0, 1 << 20) % (margin + 1)
    tallies = tallies.at[donor].add(-moved).at[sink].add(moved)
    labels = jnp.searchsorted(jnp.cumsum(tallies), jnp.arange(rows * top), side="right").astype(jnp.int32)
    listing = labels.reshape(top, rows).T
    listing = listing[jax.random.permutation(jax.random.fold_in(own, 1), rows)]
    rotation = jax.random.randint(jax.random.fold_in(own, 2), (rows, 1), 0, top)
    return jnp.take_along_axis(listing, (jnp.arange(top)[None, :] + rotation) % top, axis=1)


def load_shares(number_of, total, reach, skew, full):
    loads = [(1 << 20) // math.isqrt(standing ** skew) + 1 for standing in range(1, number_of + 1)]
    largest = reach if full else min(reach, max(-(-total // number_of), total * loads[0] // sum(loads)))
    least = 1 if total - largest >= number_of - 1 else 0
    holding, spare = [largest] + [least] * (number_of - 1), total - largest - least * (number_of - 1)
    while spare > 0:
        candidates = [i for i in range(1, number_of) if holding[i] < largest] or [i for i in range(1, number_of) if holding[i] < reach]
        whole, budget = sum([loads[i] for i in candidates]), spare
        for i in candidates:
            more = min(reach - holding[i], max(1, budget * loads[i] // whole), spare)
            holding[i] = holding[i] + more
            spare = spare - more
    return np.array(holding)


def scatter_about(own_key, shape, deviation, bound, pieces=(), kind=jnp.bfloat16):
    loudness = levels(own_key, shape, pieces, -0.22, 0.18) if pieces else 1.0
    drawn = jax.random.normal(own_key, shape, jnp.float32) * deviation * loudness
    return jnp.minimum(jnp.maximum(drawn, -bound), bound).astype(kind)


def setup_inputs(seed: int = 0) -> dict:
    key_list = jax.random.split(jax.random.key(seed), 13)
    value_in = scatter_about(key_list[0], (TOKENS_A, CW), 1.0, 6.0, ((0, 8), (1, 4)))
    gate_in = scatter_about(key_list[1], (TOKENS_A, CW), 1.0, 6.0, ((0, 8), (1, 4)))
    outer_gate = scatter_about(key_list[2], (TOKENS_A, CW), 1.0, 6.0, ((0, 8), (1, 4)))
    conv_weight = scatter_about(key_list[3], (3, CW), 3 ** -0.5, 3.5, ((1, 4),))
    out_weight = scatter_about(key_list[4], (CW, D), CW ** -0.5, 0.1875, ((0, 4),))
    moe_tokens = scatter_about(key_list[5], (TOKENS_B, D), 1.0, 6.0, ((0, 32),))
    norm_gain = jnp.clip(1.0 + 0.18 * jax.random.normal(key_list[6], (D,), jnp.float32), 0.099609375, 1.8984375).astype(jnp.bfloat16)
    routes_keys = jax.random.split(jax.random.fold_in(key_list[7], 1), TOKENS_B // TOK_DEV)
    routes_turns = jax.random.permutation(jax.random.fold_in(key_list[7], 3), TOKENS_B // TOK_DEV)
    routes = jax.vmap(lambda own, number: shared_out(jax.random.fold_in(key_list[7], 2), own, number, TOK_DEV, EXPERTS, TOP, CAP, 2))(routes_keys, routes_turns).reshape((TOKENS_B, TOP))
    route_weight = jnp.clip(0.1 + 0.9 * jax.random.uniform(key_list[8], (TOKENS_B, TOP), jnp.float32) ** levels(key_list[8], (TOKENS_B, TOP), ((0, 32),), -0.2, 0.2), 0.1, 1.0)
    expert_gate = scatter_about(key_list[9], (EXPERTS, D, FFE), D ** -0.5, 0.125, ((0, 8), (2, 4)))
    expert_up = scatter_about(key_list[10], (EXPERTS, D, FFE), D ** -0.5, 0.125, ((0, 8), (2, 4)))
    expert_down = scatter_about(key_list[11], (EXPERTS, FFE, D), FFE ** -0.5, 0.078125, ((0, 8), (1, 4)))
    return {"value_in": value_in, "gate_in": gate_in, "outer_gate": outer_gate, "conv_weight": conv_weight, "out_weight": out_weight, "moe_tokens": moe_tokens, "norm_gain": norm_gain, "routes": routes, "route_weight": route_weight, "expert_gate": expert_gate, "expert_up": expert_up, "expert_down": expert_down}


def rounded(values):
    return lax.optimization_barrier(values.astype(jnp.bfloat16)).astype(jnp.float32)

def reference(value_in, gate_in, outer_gate, conv_weight, out_weight, moe_tokens, norm_gain, routes, route_weight, expert_gate, expert_up, expert_down):
    product = (value_in.astype(jnp.float32) * gate_in.astype(jnp.float32)).astype(jnp.bfloat16)
    padded = jnp.pad(product.astype(jnp.float32), ((1, 1), (0, 0)))
    taps = conv_weight.astype(jnp.float32)
    convolved = padded[:-2] * taps[0] + padded[1:-1] * taps[1] + padded[2:] * taps[2]
    mixed_rows = (outer_gate.astype(jnp.float32) * convolved).astype(jnp.bfloat16)
    group_width = CW // N_TP
    running = jnp.zeros((TOKENS_A, D), jnp.float32)
    for group in range(N_TP):
        partial_value = jnp.dot(mixed_rows[:, group * group_width:(group + 1) * group_width], out_weight[group * group_width:(group + 1) * group_width], preferred_element_type=jnp.float32)
        running = running + rounded(partial_value)
    mixer_out = running.astype(jnp.bfloat16)
    tokens_f32 = moe_tokens.astype(jnp.float32)
    normed = (tokens_f32 * lax.rsqrt(lax.optimization_barrier(jnp.mean(tokens_f32 * tokens_f32, axis=-1, keepdims=True)) + 1e-06) * norm_gain.astype(jnp.float32)).astype(jnp.bfloat16)
    devices = TOKENS_B // TOK_DEV
    flat_ids = routes.reshape(devices, TOK_DEV * TOP)
    matches = (flat_ids[..., None] == jnp.arange(EXPERTS, dtype=jnp.int32)[None, None, :]).astype(jnp.int32)
    position = lax.optimization_barrier(jnp.sum((jnp.cumsum(matches, axis=1) - 1) * matches, axis=-1)).astype(jnp.int32)
    owners = jnp.arange(devices, dtype=jnp.int32)[:, None]
    columns = (owners * CAP + position).astype(jnp.int32)
    token_ids = jnp.broadcast_to(jnp.arange(TOKENS_B, dtype=jnp.int32).reshape(devices, TOK_DEV, 1), (devices, TOK_DEV, TOP)).reshape(devices, TOK_DEV * TOP)
    slot_table = jnp.zeros((EXPERTS, devices * CAP), jnp.int32).at[flat_ids, columns].set(token_ids + 1)
    padded_rows = jnp.concatenate([jnp.zeros((1, D), jnp.bfloat16), normed], axis=0)
    unit_width = FFE // N_TP

    def expert(operands):
        indices, gate_w, up_w, down_w = operands
        picked_rows = padded_rows[indices]
        gate_act = jnp.dot(picked_rows, gate_w, preferred_element_type=jnp.float32)
        up_act = jnp.dot(picked_rows, up_w, preferred_element_type=jnp.float32)
        hidden = (jax.nn.silu(gate_act) * up_act).astype(jnp.bfloat16)
        summed = jnp.zeros((indices.shape[0], D), jnp.float32)
        for group in range(N_TP):
            partial_value = jnp.dot(hidden[:, group * unit_width:(group + 1) * unit_width], down_w[group * unit_width:(group + 1) * unit_width], preferred_element_type=jnp.float32)
            summed = summed + rounded(partial_value)
        return summed.astype(jnp.bfloat16)
    results = lax.map(expert, (slot_table, expert_gate, expert_up, expert_down))
    where_ids = (flat_ids * (devices * CAP) + columns).reshape(TOKENS_B, TOP)
    picked = results.reshape(EXPERTS * devices * CAP, D)[where_ids].astype(jnp.float32)
    moe_out = lax.optimization_barrier(jnp.sum(route_weight[..., None] * picked, axis=1)).astype(jnp.bfloat16)
    return (mixer_out, moe_out)
```

```python
import functools

import jax
import jax.numpy as jnp
from jax import lax
from jax.experimental import pallas as pl
from jax.experimental.pallas import tpu as pltpu
from jax.sharding import PartitionSpec as P

MESH = pl.DeviceIdType.MESH
F32, BF16 = jnp.float32, jnp.bfloat16
HALO = 16
PIECES = 4


def moved(at, k, count, back=False):
    if count & (count - 1):
        return lax.rem(at + (count - k if back else k), count)
    bit = 1
    while bit < count:
        if k & bit:
            at = at + bit * (1 - 2 * lax.rem(at // bit, 2))
        bit *= 2
    return at


def paired(experts):
    near, far = list(range(2, experts // 2)), list(range(experts // 2, experts))
    left = far[len(near):]
    return [(0, 1)] + list(zip(far, near)) + list(zip(left[::2], left[1::2]))


def kernel(
    experts, shards, cap, tile,
    value_hbm, gatein_hbm, outer_hbm, conv_ref, outw_hbm, tokens_hbm, gain_ref, routes_ref, rw_ref,
    gate_hbm, up_hbm, down_hbm,
    mixer_ref, moe_ref,
    gate_w, up_w, down_w, value, gatein, outer, outw, tokens,
    normed, sent, weights, slots, hidden, part, core_in, chip_in, back,
    prod, mixed, mpart, mcore, mx_in,
    w_sem, own_sem, out_s, out_r, xf_s, xf_r, df_s, df_r, dr_s, dr_r, xr_s, xr_r, bk_s, bk_r,
    h_s, h_r, md_s, md_r, mx_s, mx_r,
):
    stages = experts // 2
    high = shards // 2
    rows_own, features = tokens.shape
    slot_count = experts * cap
    me, mine = lax.axis_index("ep"), lax.axis_index("tp")
    low, top = lax.rem(mine, 2), mine // 2
    partner = (me, mine + 1 - 2 * low)
    across = (me, lax.rem(mine + high, shards))
    wide, half = 2 * cap, 2 * high * cap
    own_half = pl.multiple_of(low * half, 16)
    other_half = pl.multiple_of((1 - low) * half, 16)
    own_top = pl.multiple_of(top * wide, 16)
    other_top = pl.multiple_of((1 - top) * wide, 16)

    def to(k):
        return moved(me, k, experts)

    def source(k):
        return moved(me, k, experts, True)

    steps = paired(experts)
    stage = {k: j for j, ks in enumerate(steps) for k in ks}
    seat = {k: ks.index(k) * cap for ks in steps for k in ks}

    def place(k):
        return pl.ds(pl.multiple_of(own_half + own_top + seat[k], 16), cap)

    def block(e):
        return pl.ds(pl.multiple_of(e * cap, 16), cap)

    def remote(src, dst, s, r, device):
        return pltpu.make_async_remote_copy(
            src_ref=src, dst_ref=dst, send_sem=s, recv_sem=r, device_id=device, device_id_type=MESH
        )

    loads = [
        pltpu.make_async_copy(a, b, w_sem.at[i])
        for i, (a, b) in enumerate(
            (
                (tokens_hbm, tokens), (value_hbm, value), (gatein_hbm, gatein),
                (outer_hbm, outer), (outw_hbm, outw),
                (gate_hbm, gate_w), (up_hbm, up_w), (down_hbm, down_w),
            )
        )
    ]
    barrier = pltpu.get_barrier_semaphore()
    for k in range(1, experts):
        pl.semaphore_signal(barrier, inc=1, device_id=(to(k), mine), device_id_type=MESH)
    for device in (partner, across):
        pl.semaphore_signal(barrier, inc=1, device_id=device, device_id_type=MESH)
    for load in loads:
        load.start()

    out = [None] + [
        remote(
            sent.at[block(to(k))], slots.at[stage[k], place(k)], out_s.at[k], out_r.at[k],
            (to(k), mine),
        )
        for k in range(1, experts)
    ]
    own_in = pltpu.make_async_copy(sent.at[block(me)], slots.at[0, place(0)], own_sem.at[0])
    x_out = [
        remote(slots.at[stage[k], place(k)], slots.at[stage[k], place(k)], xf_s.at[k], xf_r.at[k], across)
        for k in range(experts)
    ]
    rows = pl.ds(own_half, half)
    d_out = [
        remote(slots.at[j, rows], slots.at[j, rows], df_s.at[j], df_r.at[j], partner)
        for j in range(stages)
    ]
    d_back = [
        remote(part.at[j, pl.ds(other_half, half)], core_in.at[j], dr_s.at[j], dr_r.at[j], partner)
        for j in range(stages)
    ]
    x_back = [
        remote(
            core_in.at[stage[k], pl.ds(pl.multiple_of(other_top + seat[k], 16), cap)],
            chip_in.at[stage[k], pl.ds(seat[k], cap)], xr_s.at[k], xr_r.at[k], across,
        )
        for k in range(experts)
    ]
    own_out = pltpu.make_async_copy(chip_in.at[0, pl.ds(0, cap)], back.at[block(me)], own_sem.at[1])
    home = [own_out] + [
        remote(
            chip_in.at[stage[k], pl.ds(seat[k], cap)], back.at[block(me)],
            bk_s.at[k], bk_r.at[k], (source(k), mine),
        )
        for k in range(1, experts)
    ]
    length = value.shape[0]
    halo = [
        remote(
            prod.at[pl.ds(length, HALO)], prod.at[pl.ds(0, HALO)], h_s.at[0], h_r.at[0],
            (lax.rem(me + 1, experts), mine),
        ),
        remote(
            prod.at[pl.ds(HALO, HALO)], prod.at[pl.ds(length + HALO, HALO)], h_s.at[1], h_r.at[1],
            (lax.rem(me + experts - 1, experts), mine),
        ),
    ]
    owned = length // shards

    def owner_rows(x, core):
        return pl.ds(pl.multiple_of((2 * x + core) * owned, 16), owned)

    m_core = [
        remote(
            mpart.at[owner_rows(x, 1 - low)], mcore.at[x], md_s.at[x], md_r.at[x], partner
        )
        for x in range(high)
    ]
    piece = owned // PIECES
    m_across = [
        remote(
            mcore.at[1 - top, pl.ds(i * piece, piece)], mx_in.at[pl.ds(i * piece, piece)],
            mx_s.at[i], mx_r.at[i], across,
        )
        for i in range(PIECES)
    ]

    loads[0].wait()
    gain = gain_ref[...].astype(F32)

    def norm(i, carry):
        at = pl.ds(pl.multiple_of(i * 16, 16), 16)
        x = tokens[at, :].astype(F32)
        scale = lax.rsqrt(jnp.mean(x * x, axis=-1, keepdims=True) + 1e-06)
        normed[at, :] = (x * scale * gain).astype(BF16)
        return carry

    lax.fori_loop(0, rows_own // 16, norm, 0)
    width = 128 * (-(-experts // 128))
    lanes = lax.broadcasted_iota(jnp.int32, (rows_own, width), 1)
    first, second = routes_ref[:, 0:1], routes_ref[:, 1:2]
    is_first = (lanes == first).astype(F32)
    is_second = (lanes == second).astype(F32)
    named = (is_first + is_second).astype(BF16)
    before = (
        lax.broadcasted_iota(jnp.int32, (rows_own, rows_own), 0)
        > lax.broadcasted_iota(jnp.int32, (rows_own, rows_own), 1)
    )
    rank = jnp.dot(before.astype(F32).astype(BF16), named, preferred_element_type=F32)
    slot_lanes = lax.broadcasted_iota(jnp.int32, (rows_own, slot_count), 1).astype(F32)

    def at_slot(route, chosen):
        position = jnp.sum(chosen * rank, axis=1, keepdims=True)
        return (slot_lanes == route.astype(F32) * cap + position).astype(F32)

    at_first, at_second = at_slot(first, is_first), at_slot(second, is_second)
    placement = (at_first + at_second).astype(BF16)

    def gather(i, carry):
        at = pl.ds(pl.multiple_of(i * tile, tile), tile)
        sent[:, at] = lax.dot_general(
            placement, normed[:, at], (((0,), (0,)), ((), ())), preferred_element_type=F32
        ).astype(BF16)
        return carry

    lax.fori_loop(0, features // tile, gather, 0)
    mix = at_first * rw_ref[:, 0:1] + at_second * rw_ref[:, 1:2]
    leading = mix.astype(BF16)
    weights[pl.ds(0, rows_own), :] = leading
    weights[pl.ds(rows_own, rows_own), :] = (mix - leading.astype(F32)).astype(BF16)

    loads[1].wait()
    loads[2].wait()
    prod[pl.ds(HALO, length), :] = (value[...].astype(F32) * gatein[...].astype(F32)).astype(BF16)
    pl.semaphore_wait(barrier, experts + 1)
    for copy in halo:
        copy.start()
    own_in.start()
    for ks in steps[1:] + [(1,)]:
        for k in ks:
            out[k].start()
    own_in.wait()
    x_out[0].start()

    loads[3].wait()
    loads[4].wait()
    for copy in halo:
        copy.wait()
    keep_first = jnp.where(me == 0, 0.0, 1.0)
    keep_last = jnp.where(me == experts - 1, 0.0, 1.0)
    prod[pl.ds(0, HALO), :] = (prod[pl.ds(0, HALO), :].astype(F32) * keep_first).astype(BF16)
    last = pl.ds(length + HALO, HALO)
    prod[last, :] = (prod[last, :].astype(F32) * keep_last).astype(BF16)
    taps = conv_ref[...].astype(F32)

    def mix_rows(x, core):
        start = pl.multiple_of((2 * x + core) * owned, 16)
        span = owned + 2 * HALO
        p = prod[pl.ds(start, span), :].astype(F32)
        convolved = (
            pltpu.roll(p, 1, 0) * taps[0:1] + p * taps[1:2] + pltpu.roll(p, span - 1, 0) * taps[2:3]
        )[HALO:HALO + owned]
        mixed[...] = (outer[pl.ds(start, owned), :].astype(F32) * convolved).astype(BF16)

        def step(i, carry):
            at = pl.ds(pl.multiple_of(i * tile, tile), tile)
            mpart[pl.ds(start, owned), at] = jnp.dot(
                mixed[...], outw[:, at], preferred_element_type=F32
            ).astype(BF16)
            return carry

        lax.fori_loop(0, features // tile, step, 0)

    for x in range(high):
        mix_rows(x, 1 - low)
        m_core[x].start()

    def arrive(k):
        out[k].wait_recv()
        x_out[k].start()

    arrive(1)
    for x in range(high):
        mix_rows(x, low)
    for x in range(high):
        m_core[x].wait_recv()

    def sum_across(i):
        at = pl.ds(i * piece, piece)
        theirs = pl.ds(pl.multiple_of((2 * (1 - top) + low) * owned + i * piece, 16), piece)
        mcore[1 - top, at] = (
            mcore[1 - top, at].astype(F32) + mpart[theirs, :].astype(F32)
        ).astype(BF16)

    for i in range(PIECES):
        sum_across(i)
    m_across[0].start()

    def spread(j):
        for k in steps[j]:
            x_out[k].wait_recv()
        d_out[j].start()

    def activate(j, hooks):
        d_out[j].wait_recv()

        def step(i, carry):
            for at_step, hook in hooks:
                @pl.when(i == at_step)
                def _():
                    hook()

            at = pl.ds(pl.multiple_of(i * tile, tile), tile)
            x = slots[j]
            g = jnp.dot(x, gate_w[:, at], preferred_element_type=F32)
            u = jnp.dot(x, up_w[:, at], preferred_element_type=F32)
            hidden[:, at] = (g / (1.0 + jnp.exp(-g)) * u).astype(BF16)
            return carry

        lax.fori_loop(0, gate_w.shape[1] // tile, step, 0)

    def project(j):
        def step(i, carry):
            at = pl.ds(pl.multiple_of(i * tile, tile), tile)
            part[j, :, at] = jnp.dot(
                hidden[...], down_w[:, at], preferred_element_type=F32
            ).astype(BF16)
            return carry

        lax.fori_loop(0, down_w.shape[1] // tile, step, 0)
        d_back[j].start()

    def pair_up(j):
        d_back[j].wait_recv()
        for k in steps[j]:
            def step(i, carry):
                first = pl.multiple_of(other_top + seat[k] + i * 16, 16)
                at = pl.ds(first, 16)
                theirs = pl.ds(pl.multiple_of(own_half + first, 16), 16)
                core_in[j, at] = (
                    part[j, theirs].astype(F32) + core_in[j, at].astype(F32)
                ).astype(BF16)
                return carry

            lax.fori_loop(0, cap // 16, step, 0)
            x_back[k].start()

    def finish(k):
        j = stage[k]
        x_back[k].wait_recv()

        def step(i, carry):
            here = pl.ds(pl.multiple_of(seat[k] + i * 16, 16), 16)
            first = pl.multiple_of(own_top + seat[k] + i * 16, 16)
            held = pl.ds(pl.multiple_of(own_half + first, 16), 16)
            chip_in[j, here] = (
                part[j, held].astype(F32)
                + core_in[j, pl.ds(first, 16)].astype(F32)
                + chip_in[j, here].astype(F32)
            ).astype(BF16)
            return carry

        lax.fori_loop(0, cap // 16, step, 0)
        home[k].start()

    def arrive_all(j):
        for k in steps[j] if j < stages else ():
            arrive(k)

    arrive_all(1)
    spread(0)
    for i in range(stages):
        hooks = []
        if i == stages - 2:
            hooks.append((1, functools.partial(arrive, steps[-1][1])))
        if i >= 2:
            hooks.append((2, functools.partial(pair_up, i - 1)))
        if i == 0:
            loads[5].wait()
            loads[6].wait()
        activate(i, hooks)
        if i + 2 == stages - 1:
            arrive(steps[-1][0])
        else:
            arrive_all(i + 2)
        if i >= 3:
            for k in steps[i - 2]:
                finish(k)
        if i >= 1 and i + 1 < stages:
            spread(i + 1)
        if i == 0:
            loads[7].wait()
        project(i)
        if i == 0:
            spread(1)
    pair_up(stages - 1)
    pair_up(0)
    for i in range(1, PIECES):
        m_across[i].start()
    for j in (stages - 2, stages - 1, 0):
        for k in steps[j]:
            finish(k)

    for i in range(PIECES):
        m_across[i].wait_recv()
    mine_rows = pl.multiple_of(mine * owned, 16)

    def sum_own(i, carry):
        at = pl.ds(pl.multiple_of(i * 16, 16), 16)
        mixer_ref[at, :] = (
            mpart[pl.ds(pl.multiple_of(mine_rows + i * 16, 16), 16), :].astype(F32)
            + mcore[top, at].astype(F32)
            + mx_in[at, :].astype(F32)
        ).astype(BF16)
        return carry

    lax.fori_loop(0, owned // 16, sum_own, 0)
    own_out.wait()
    for k in range(1, experts):
        home[k].wait()

    def combine(i, carry):
        at = pl.ds(pl.multiple_of(i * tile, tile), tile)
        both = jnp.dot(weights[...], back[:, at], preferred_element_type=F32)
        moe_ref[:, at] = (both[:rows_own] + both[rows_own:]).astype(BF16)
        return carry

    lax.fori_loop(0, features // tile, combine, 0)
    for k in range(1, experts):
        out[k].wait_send()
    for k in range(experts):
        x_out[k].wait_send()
        x_back[k].wait_send()
    for j in range(stages):
        d_out[j].wait_send()
        d_back[j].wait_send()
    for copy in m_core + m_across:
        copy.wait_send()


def body(
    value_in, gate_in, outer_gate, conv_weight, out_weight, moe_tokens, norm_gain, routes,
    route_weight, expert_gate, expert_up, expert_down,
):
    row_total, top_count = routes.shape
    features = moe_tokens.shape[1]
    length, channels = value_in.shape
    local_units = expert_gate.shape[2]
    experts, shards = lax.axis_size("ep"), lax.axis_size("tp")
    capacity = 3 * top_count * row_total // (2 * experts)
    capacity = -(-capacity // 16) * 16
    slots = experts * capacity
    stages, rows = experts // 2, 2 * shards * capacity
    owned = length // shards
    dma = pltpu.SemaphoreType.DMA
    vmem, hbm = pl.BlockSpec(memory_space=pltpu.VMEM), pl.BlockSpec(memory_space=pl.ANY)
    return pl.pallas_call(
        functools.partial(kernel, experts, shards, capacity, 512),
        out_shape=(
            jax.ShapeDtypeStruct((owned, features), BF16),
            jax.ShapeDtypeStruct((row_total, features), BF16),
        ),
        in_specs=[hbm, hbm, hbm, vmem, hbm, hbm, vmem, vmem, vmem, hbm, hbm, hbm],
        out_specs=(vmem, vmem),
        scratch_shapes=[
            pltpu.VMEM((features, local_units), BF16),
            pltpu.VMEM((features, local_units), BF16),
            pltpu.VMEM((local_units, features), BF16),
            pltpu.VMEM((length, channels), BF16),
            pltpu.VMEM((length, channels), BF16),
            pltpu.VMEM((length, channels), BF16),
            pltpu.VMEM((channels, features), BF16),
            pltpu.VMEM((row_total, features), BF16),
            pltpu.VMEM((row_total, features), BF16),
            pltpu.VMEM((slots, features), BF16),
            pltpu.VMEM((2 * row_total, slots), BF16),
            pltpu.VMEM((stages, rows, features), BF16),
            pltpu.VMEM((rows, local_units), BF16),
            pltpu.VMEM((stages, rows, features), BF16),
            pltpu.VMEM((stages, rows // 2, features), BF16),
            pltpu.VMEM((stages, rows // shards, features), BF16),
            pltpu.VMEM((slots, features), BF16),
            pltpu.VMEM((length + 2 * HALO, channels), BF16),
            pltpu.VMEM((owned, channels), BF16),
            pltpu.VMEM((length, features), BF16),
            pltpu.VMEM((shards // 2, owned, features), BF16),
            pltpu.VMEM((owned, features), BF16),
            dma((8,)),
            dma((2,)),
        ]
        + [dma((experts,))] * 4
        + [dma((stages,))] * 4
        + [dma((experts,))] * 4
        + [dma((2,))] * 4
        + [dma((PIECES,))] * 2,
        compiler_params=pltpu.CompilerParams(
            collective_id=0, has_side_effects=True, vmem_limit_bytes=67043328
        ),
        cost_estimate=pl.CostEstimate(
            flops=6 * stages * rows * features * local_units,
            bytes_accessed=6 * features * local_units,
            transcendentals=stages * rows * local_units,
        ),
    )(
        value_in, gate_in, outer_gate, conv_weight, out_weight, moe_tokens,
        norm_gain.reshape(1, features), routes, route_weight,
        expert_gate[0], expert_up[0], expert_down[0],
    )


def solution(mesh):
    placed = (
        P("ep", "tp"),
        P("ep", "tp"),
        P("ep", "tp"),
        P(None, "tp"),
        P("tp", None),
        P(("ep", "tp"), None),
        P(),
        P(("ep", "tp"), None),
        P(("ep", "tp"), None),
        P("ep", None, "tp"),
        P("ep", None, "tp"),
        P("ep", "tp", None),
    )
    return jax.shard_map(
        body,
        mesh=mesh,
        in_specs=placed,
        out_specs=(P(("ep", "tp"), None), P(("ep", "tp"), None)),
        check_vma=False,
    )
```

```python
import functools

import jax
import jax.numpy as jnp
from jax import lax
from jax.experimental import pallas as pl
from jax.experimental.pallas import tpu as pltpu
from jax.sharding import PartitionSpec as P

MESH = pl.DeviceIdType.MESH
F32, BF16 = jnp.float32, jnp.bfloat16
HALO = 16
PIECES = (1, 3)


def moved(at, k, count, back=False):
    if count & (count - 1):
        return lax.rem(at + (count - k if back else k), count)
    bit = 1
    while bit < count:
        if k & bit:
            at = at + bit * (1 - 2 * lax.rem(at // bit, 2))
        bit *= 2
    return at


def paired(experts):
    near, far = list(range(2, experts // 2)), list(range(experts // 2, experts))
    steps = [(0, 1)]
    for i in range(0, len(near), 2):
        steps += [(far[i],), (far[i + 1],), tuple(near[i:i + 2])]
    return steps + [(k,) for k in far[len(near):]]


def sequence(experts):
    near, far = list(range(2, experts // 2)), list(range(experts // 2, experts))
    both = [k for pair in zip(far, near) for k in pair]
    return both + far[len(near):]


def kernel(
    experts, shards, cap, tile,
    value_hbm, gatein_hbm, outer_hbm, conv_hbm, outw_hbm, tokens_hbm, gain_hbm, routes_hbm, rw_hbm,
    gate_hbm, up_hbm, down_hbm,
    mixer_ref, moe_ref,
    gate_w, up_w, down_w, value, gatein, outer, outw, tokens, conv_ref, gain_ref, routes_ref, rw_ref,
    routes_in, rw_in, normed, sent, weights, weights_in, slots, hidden, part, core_in, chip_in,
    back, back_in, cross_out, cross_in,
    prod, mixed, mpart, mcore, mx_in,
    w_sem, own_sem, out_s, out_r, xf_s, xf_r, df_s, df_r, dr_s, dr_r, xr_s, xr_r, bk_s, bk_r,
    h_s, h_r, md_s, md_r, mx_s, mx_r, rt_s, rt_r, pk_s, pk_r, cx_s, cx_r,
):
    high = shards // 2
    rows_own, features = tokens.shape
    slot_count = experts * cap
    me, mine = lax.axis_index("ep"), lax.axis_index("tp")
    low, top = lax.rem(mine, 2), mine // 2
    partner = (me, mine + 1 - 2 * low)
    across = (me, lax.rem(mine + high, shards))

    def to(k):
        return moved(me, k, experts)

    def source(k):
        return moved(me, k, experts, True)

    steps = paired(experts)
    stages = len(steps)
    stage = {k: j for j, ks in enumerate(steps) for k in ks}
    seat = {k: ks.index(k) * cap for ks in steps for k in ks}
    wide = [cap * len(ks) for ks in steps]
    half = [high * w for w in wide]
    base = [2 * sum(half[:j]) for j in range(stages)]
    part_base = [sum(half[:j]) for j in range(stages)]

    near = experts // 2
    first_near = (me // near) * near

    def rows_at(first, count):
        return pl.ds(pl.multiple_of(first, 16), count)

    def own_rows(j):
        return base[j] + low * half[j]

    def place(k):
        j = stage[k]
        return rows_at(own_rows(j) + top * wide[j] + seat[k], cap)

    def block(e):
        return pl.ds(pl.multiple_of(e * cap, 16), cap)

    def remote(src, dst, s, r, device):
        return pltpu.make_async_remote_copy(
            src_ref=src, dst_ref=dst, send_sem=s, recv_sem=r, device_id=device, device_id_type=MESH
        )

    barrier = pltpu.get_barrier_semaphore()
    for k in range(1, experts):
        pl.semaphore_signal(barrier, inc=1, device_id=(to(k), mine), device_id_type=MESH)
    for device in (partner, across):
        pl.semaphore_signal(barrier, inc=1, device_id=device, device_id_type=MESH)
    wanted = (
        (tokens_hbm, tokens), (gain_hbm, gain_ref), (routes_hbm, routes_ref),
        (value_hbm, value), (gatein_hbm, gatein), (outer_hbm, outer), (outw_hbm, outw),
        (conv_hbm, conv_ref), (rw_hbm, rw_ref),
        (gate_hbm, gate_w), (up_hbm, up_w), (down_hbm, down_w),
    )
    loads = [pltpu.make_async_copy(a, b, w_sem.at[i]) for i, (a, b) in enumerate(wanted)]
    for load in loads:
        load.start()

    out = [None] + [
        remote(
            sent.at[block(to(k))], slots.at[place(k)], out_s.at[k], out_r.at[k],
            (to(k), mine),
        )
        for k in range(1, experts)
    ]
    own_in = pltpu.make_async_copy(sent.at[block(me)], slots.at[place(0)], own_sem.at[0])
    groups = [(k,) for k in range(experts)]

    def crossing(i, ks):
        j = stage[ks[0]]
        here = slots.at[rows_at(own_rows(j) + top * wide[j] + seat[ks[0]], cap * len(ks))]
        return remote(
            here if ks[0] else sent.at[block(me)], here, xf_s.at[i], xf_r.at[i], across
        )

    x_out = {ks: crossing(i, ks) for i, ks in enumerate(groups)}

    def to_partner(j):
        here = slots.at[rows_at(own_rows(j), half[j])]
        return remote(here, here, df_s.at[j], df_r.at[j], partner)

    d_out = [to_partner(j) for j in range(stages)]
    d_back = [
        remote(
            part.at[rows_at(base[j] + (1 - low) * half[j], half[j])],
            core_in.at[rows_at(part_base[j], half[j])], dr_s.at[j], dr_r.at[j], partner,
        )
        for j in range(stages)
    ]
    def core_rows(k, of):
        j = stage[k]
        return core_in.at[rows_at(part_base[j] + of * wide[j] + seat[k], cap)]

    def chip_rows(k):
        return rows_at((k - near) * cap, cap)

    x_back = {
        k: remote(
            core_rows(k, 1 - top), chip_in.at[chip_rows(k)],
            xr_s.at[k - near], xr_r.at[k - near], across,
        )
        for k in range(near, experts)
    }
    home = {
        k: remote(
            chip_in.at[chip_rows(k)] if k >= near else core_rows(k, top), back.at[block(me)],
            bk_s.at[k], bk_r.at[k], (source(k), mine),
        )
        for k in range(1, experts)
    }
    home_in = {
        k: remote(
            core_rows(k, 1 - top), back_in.at[block(me - first_near)],
            pk_s.at[k], pk_r.at[k], (source(k), mine),
        )
        for k in range(1, near)
    }
    cross = remote(cross_out, cross_in, cx_s.at[0], cx_r.at[0], across)
    routing = [
        remote(routes_ref, routes_in, rt_s.at[0], rt_r.at[0], across),
        remote(rw_ref, rw_in, rt_s.at[1], rt_r.at[1], across),
    ]
    length = value.shape[0]
    halo = [
        remote(
            prod.at[pl.ds(length, HALO)], prod.at[pl.ds(0, HALO)], h_s.at[0], h_r.at[0],
            (lax.rem(me + 1, experts), mine),
        ),
        remote(
            prod.at[pl.ds(HALO, HALO)], prod.at[pl.ds(length + HALO, HALO)], h_s.at[1], h_r.at[1],
            (lax.rem(me + experts - 1, experts), mine),
        ),
    ]
    owned = length // shards

    def owner_rows(x, core):
        return pl.ds(pl.multiple_of((2 * x + core) * owned, 16), owned)

    m_core = [
        remote(
            mpart.at[owner_rows(x, 1 - low)], mcore.at[x], md_s.at[x], md_r.at[x], partner
        )
        for x in range(high)
    ]
    unit = owned // sum(PIECES)
    pieces = [pl.ds(sum(PIECES[:i]) * unit, count * unit) for i, count in enumerate(PIECES)]
    m_across = [
        remote(mcore.at[1 - top, at], mx_in.at[at], mx_s.at[i], mx_r.at[i], across)
        for i, at in enumerate(pieces)
    ]

    for load in loads[:3]:
        load.wait()
    gain = gain_ref[...].astype(F32).reshape(1, features)

    def norm(i, carry):
        at = pl.ds(pl.multiple_of(i * 32, 32), 32)
        x = tokens[at, :].astype(F32)
        scale = lax.rsqrt(jnp.mean(x * x, axis=-1, keepdims=True) + 1e-06)
        normed[at, :] = (x * scale * gain).astype(BF16)
        return carry

    lax.fori_loop(0, rows_own // 32, norm, 0)
    lines = 16 * (-(-experts // 16))
    expert_ids = lax.broadcasted_iota(jnp.int32, (lines, rows_own), 0)
    before = (
        lax.broadcasted_iota(jnp.int32, (rows_own, rows_own), 0)
        < lax.broadcasted_iota(jnp.int32, (rows_own, rows_own), 1)
    ).astype(F32).astype(BF16)

    def slots_of(routes, start, count):
        chosen = [(expert_ids == routes[i:i + 1, :]).astype(F32) for i in range(2)]
        named = (chosen[0] + chosen[1]).astype(BF16)
        rank = jnp.dot(named, before, preferred_element_type=F32)
        ids = (lax.broadcasted_iota(jnp.int32, (count, rows_own), 0) + start).astype(F32)

        def at_slot(i):
            position = jnp.sum(chosen[i] * rank, axis=0, keepdims=True)
            return (ids == routes[i:i + 1, :].astype(F32) * cap + position).astype(F32)

        return at_slot(0), at_slot(1)

    def weigh(ref, at_first, at_second, rw):
        mix = at_first * rw[0:1, :] + at_second * rw[1:2, :]
        leading = mix.astype(BF16).astype(F32)
        ref[pl.ds(0, rows_own), :] = leading.T.astype(BF16)
        ref[pl.ds(rows_own, rows_own), :] = (mix - leading).T.astype(BF16)

    at_first, at_second = slots_of(routes_ref[...], 0, slot_count)
    placement = (at_first + at_second).astype(BF16)

    def gather(i, carry):
        at = pl.ds(pl.multiple_of(i * tile, tile), tile)
        sent[:, at] = jnp.dot(
            placement, normed[:, at], preferred_element_type=F32
        ).astype(BF16)
        return carry

    lax.fori_loop(0, features // tile, gather, 0)
    loads[3].wait()
    loads[4].wait()

    def multiply(first, count):
        at = pl.ds(first, count)
        prod[pl.ds(HALO + first, count), :] = (
            value[at, :].astype(F32) * gatein[at, :].astype(F32)
        ).astype(BF16)

    multiply(0, HALO)
    multiply(length - HALO, HALO)
    pl.semaphore_wait(barrier, experts + 1)
    x_out[0,].start()
    loads[8].wait()
    for copy in routing:
        copy.start()
    for copy in halo:
        copy.start()
    for k in sequence(experts) + [1]:
        out[k].start()
    own_in.start()

    multiply(HALO, length - 2 * HALO)
    for load in loads[5:8]:
        load.wait()
    for copy in halo:
        copy.wait()
    keep_first = jnp.where(me == 0, 0.0, 1.0)
    keep_last = jnp.where(me == experts - 1, 0.0, 1.0)
    prod[pl.ds(0, HALO), :] = (prod[pl.ds(0, HALO), :].astype(F32) * keep_first).astype(BF16)
    last = pl.ds(length + HALO, HALO)
    prod[last, :] = (prod[last, :].astype(F32) * keep_last).astype(BF16)
    taps = conv_ref[...].astype(F32)

    def mix_rows(x, core):
        start = pl.multiple_of((2 * x + core) * owned, 16)
        span = owned + 2 * HALO
        p = prod[pl.ds(start, span), :].astype(F32)
        convolved = (
            pltpu.roll(p, 1, 0) * taps[0:1] + p * taps[1:2] + pltpu.roll(p, span - 1, 0) * taps[2:3]
        )[HALO:HALO + owned]
        mixed[...] = (outer[pl.ds(start, owned), :].astype(F32) * convolved).astype(BF16)

        def step(i, carry):
            at = pl.ds(pl.multiple_of(i * tile, tile), tile)
            mpart[pl.ds(start, owned), at] = jnp.dot(
                mixed[...], outw[:, at], preferred_element_type=F32
            ).astype(BF16)
            return carry

        lax.fori_loop(0, features // tile, step, 0)

    for x in range(high):
        mix_rows(x, 1 - low)
        m_core[x].start()

    weigh(weights, at_first, at_second, rw_ref[...])
    own_in.wait()

    def arrive(*ks):
        for k in ks:
            out[k].wait_recv()
        x_out[ks].start()

    arrive(1)
    for x in range(high):
        mix_rows(x, low)
    for x in range(high):
        m_core[x].wait_recv()

    theirs = pl.multiple_of((2 * (1 - top) + low) * owned, 16)

    def sum_across(i, carry):
        at = pl.ds(pl.multiple_of(i * 16, 16), 16)
        mcore[1 - top, at] = (
            mcore[1 - top, at].astype(F32)
            + mpart[pl.ds(pl.multiple_of(theirs + i * 16, 16), 16), :].astype(F32)
        ).astype(BF16)
        return carry

    lax.fori_loop(0, owned // 16, sum_across, 0)
    m_across[0].start()

    def spread(j):
        for ks in groups:
            if stage[ks[0]] == j:
                x_out[ks].wait_recv()
        d_out[j].start()

    def activate(j, hooks):
        d_out[j].wait_recv()

        def step(i, carry):
            for at_step, hook in hooks:
                @pl.when(i == at_step)
                def _():
                    hook()

            at = pl.ds(pl.multiple_of(i * tile, tile), tile)
            x = slots[pl.ds(base[j], 2 * half[j]), :]
            g = jnp.dot(x, gate_w[:, at], preferred_element_type=F32)
            u = jnp.dot(x, up_w[:, at], preferred_element_type=F32)
            hidden[pl.ds(0, 2 * half[j]), at] = (g / (1.0 + jnp.exp(-g)) * u).astype(BF16)
            return carry

        lax.fori_loop(0, gate_w.shape[1] // tile, step, 0)

    def project(j):
        def step(i, carry):
            at = pl.ds(pl.multiple_of(i * tile, tile), tile)
            part[pl.ds(base[j], 2 * half[j]), at] = jnp.dot(
                hidden[pl.ds(0, 2 * half[j]), :], down_w[:, at], preferred_element_type=F32
            ).astype(BF16)
            return carry

        lax.fori_loop(0, down_w.shape[1] // tile, step, 0)
        d_back[j].start()

    def pair_sum(k, of, ref, start):
        j = stage[k]

        def step(i, carry):
            first = of * wide[j] + seat[k] + i * 16
            ref[rows_at(start + i * 16, 16), :] = (
                part[rows_at(own_rows(j) + first, 16), :].astype(F32)
                + core_in[rows_at(part_base[j] + first, 16), :].astype(F32)
            ).astype(BF16)
            return carry

        lax.fori_loop(0, cap // 16, step, 0)

    def pair_up(j):
        d_back[j].wait_recv()
        for k in steps[j]:
            at = part_base[j] + seat[k]
            if k == 0:
                pair_sum(k, top, back, me * cap)
                pair_sum(k, 1 - top, back_in, (me - first_near) * cap)
                continue
            pair_sum(k, 1 - top, core_in, at + (1 - top) * wide[j])
            if k >= near:
                x_back[k].start()
                continue
            home_in[k].start()
            pair_sum(k, top, core_in, at + top * wide[j])
            home[k].start()

    def finish(k):
        j = stage[k]
        x_back[k].wait_recv()

        def step(i, carry):
            here = rows_at((k - near) * cap + i * 16, 16)
            first = top * wide[j] + seat[k] + i * 16
            chip_in[here, :] = (
                part[rows_at(own_rows(j) + first, 16), :].astype(F32)
                + core_in[rows_at(part_base[j] + first, 16), :].astype(F32)
                + chip_in[here, :].astype(F32)
            ).astype(BF16)
            return carry

        lax.fori_loop(0, cap // 16, step, 0)
        home[k].start()

    def finish_all(j):
        for k in steps[j]:
            if k >= near:
                finish(k)

    waiting = sequence(experts)

    def arrive_to(j):
        while any(k in waiting for ks in steps[:j + 1] for k in ks):
            arrive(waiting.pop(0))

    for k in range(2):
        arrive(waiting.pop(0))
    spread(0)
    for copy in routing:
        copy.wait_recv()
    weigh(
        weights_in, *slots_of(routes_in[...], first_near * cap, near * cap), rw_in[...]
    )
    for i in range(stages):
        hooks = []
        if i == 0:
            hooks.append((2, functools.partial(spread, 1)))
            loads[9].wait()
            loads[10].wait()
        else:
            hooks.append((1, functools.partial(arrive_to, i + 2)))
            hooks.append((2, functools.partial(pair_up, i - 1)))
        activate(i, hooks)
        if i == 0:
            arrive_to(2)
            loads[11].wait()
        elif i + 1 < stages:
            spread(i + 1)
        if i == 3:
            finish_all(1)
        project(i)
        if i > 3:
            finish_all(i - 2)
    pair_up(stages - 1)
    for copy in m_across[1:]:
        copy.start()
    finish_all(stages - 2)
    finish_all(stages - 1)
    for k in range(1, near):
        home_in[k].wait_recv()

    def combine_in(i, carry):
        at = pl.ds(pl.multiple_of(i * tile, tile), tile)
        both = jnp.dot(weights_in[...], back_in[:, at], preferred_element_type=F32)
        cross_out[:, at] = (both[:rows_own] + both[rows_own:]).astype(BF16)
        return carry

    lax.fori_loop(0, features // tile, combine_in, 0)
    cross.start()

    for copy in m_across:
        copy.wait_recv()
    mine_rows = pl.multiple_of(mine * owned, 16)

    def sum_own(i, carry):
        at = pl.ds(pl.multiple_of(i * 16, 16), 16)
        mixer_ref[at, :] = (
            mpart[pl.ds(pl.multiple_of(mine_rows + i * 16, 16), 16), :].astype(F32)
            + mcore[top, at].astype(F32)
            + mx_in[at, :].astype(F32)
        ).astype(BF16)
        return carry

    lax.fori_loop(0, owned // 16, sum_own, 0)
    for k in range(1, experts):
        home[k].wait()
    cross.wait()

    def combine(i, carry):
        at = pl.ds(pl.multiple_of(i * tile, tile), tile)
        both = jnp.dot(weights[...], back[:, at], preferred_element_type=F32)
        moe_ref[:, at] = (
            both[:rows_own] + both[rows_own:] + cross_in[:, at].astype(F32)
        ).astype(BF16)
        return carry

    lax.fori_loop(0, features // tile, combine, 0)
    for k in range(1, experts):
        out[k].wait_send()
    for copy in list(x_out.values()) + list(x_back.values()) + list(home_in.values()) + routing:
        copy.wait_send()
    for j in range(stages):
        d_out[j].wait_send()
        d_back[j].wait_send()
    for copy in m_core + m_across:
        copy.wait_send()


def body(
    value_in, gate_in, outer_gate, conv_weight, out_weight, moe_tokens, norm_gain, routes,
    route_weight, expert_gate, expert_up, expert_down,
):
    row_total, top_count = routes.shape
    features = moe_tokens.shape[1]
    length, channels = value_in.shape
    local_units = expert_gate.shape[2]
    experts, shards = lax.axis_size("ep"), lax.axis_size("tp")
    capacity = 3 * top_count * row_total // (2 * experts)
    capacity = -(-capacity // 16) * 16
    slots = experts * capacity
    steps = paired(experts)
    stages, total = len(steps), slots * shards
    owned = length // shards
    dma = pltpu.SemaphoreType.DMA
    vmem, hbm = pl.BlockSpec(memory_space=pltpu.VMEM), pl.BlockSpec(memory_space=pl.ANY)
    return pl.pallas_call(
        functools.partial(kernel, experts, shards, capacity, 512),
        out_shape=(
            jax.ShapeDtypeStruct((owned, features), BF16),
            jax.ShapeDtypeStruct((row_total, features), BF16),
        ),
        in_specs=[hbm] * 12,
        out_specs=(vmem, vmem),
        scratch_shapes=[
            pltpu.VMEM((features, local_units), BF16),
            pltpu.VMEM((features, local_units), BF16),
            pltpu.VMEM((local_units, features), BF16),
            pltpu.VMEM((length, channels), BF16),
            pltpu.VMEM((length, channels), BF16),
            pltpu.VMEM((length, channels), BF16),
            pltpu.VMEM((channels, features), BF16),
            pltpu.VMEM((row_total, features), BF16),
            pltpu.VMEM(conv_weight.shape, BF16),
            pltpu.VMEM(norm_gain.shape, BF16),
            pltpu.VMEM((top_count, row_total), jnp.int32),
            pltpu.VMEM((top_count, row_total), F32),
            pltpu.VMEM((top_count, row_total), jnp.int32),
            pltpu.VMEM((top_count, row_total), F32),
            pltpu.VMEM((row_total, features), BF16),
            pltpu.VMEM((slots, features), BF16),
            pltpu.VMEM((2 * row_total, slots), BF16),
            pltpu.VMEM((2 * row_total, slots // 2), BF16),
            pltpu.VMEM((total, features), BF16),
            pltpu.VMEM((2 * shards * capacity, local_units), BF16),
            pltpu.VMEM((total, features), BF16),
            pltpu.VMEM((total // 2, features), BF16),
            pltpu.VMEM((slots // 2, features), BF16),
            pltpu.VMEM((slots, features), BF16),
            pltpu.VMEM((slots // 2, features), BF16),
            pltpu.VMEM((row_total, features), BF16),
            pltpu.VMEM((row_total, features), BF16),
            pltpu.VMEM((length + 2 * HALO, channels), BF16),
            pltpu.VMEM((owned, channels), BF16),
            pltpu.VMEM((length, features), BF16),
            pltpu.VMEM((shards // 2, owned, features), BF16),
            pltpu.VMEM((owned, features), BF16),
            dma((12,)),
            dma((1,)),
        ]
        + [dma((experts,))] * 4
        + [dma((stages,))] * 4
        + [dma((experts,))] * 4
        + [dma((2,))] * 4
        + [dma((len(PIECES),))] * 2
        + [dma((2,))] * 2
        + [dma((experts // 2,))] * 2
        + [dma((1,))] * 2,
        compiler_params=pltpu.CompilerParams(
            collective_id=0, has_side_effects=True, vmem_limit_bytes=67043328
        ),
        cost_estimate=pl.CostEstimate(
            flops=6 * total * features * local_units,
            bytes_accessed=6 * features * local_units,
            transcendentals=total * local_units,
        ),
    )(
        value_in, gate_in, outer_gate, conv_weight, out_weight, moe_tokens,
        norm_gain, routes.T, route_weight.T,
        expert_gate[0], expert_up[0], expert_down[0],
    )


def solution(mesh):
    placed = (
        P("ep", "tp"),
        P("ep", "tp"),
        P("ep", "tp"),
        P(None, "tp"),
        P("tp", None),
        P(("ep", "tp"), None),
        P(),
        P(("ep", "tp"), None),
        P(("ep", "tp"), None),
        P("ep", None, "tp"),
        P("ep", None, "tp"),
        P("ep", "tp", None),
    )
    return jax.shard_map(
        body,
        mesh=mesh,
        in_specs=placed,
        out_specs=(P(("ep", "tp"), None), P(("ep", "tp"), None)),
        check_vma=False,
    )
```

```python
import functools

import jax
import jax.numpy as jnp
from jax import lax
from jax.experimental import pallas as pl
from jax.experimental.pallas import tpu as pltpu
from jax.sharding import PartitionSpec as P

MESH = pl.DeviceIdType.MESH
F32, BF16 = jnp.float32, jnp.bfloat16
HALO = 16
PIECES = (1, 3)


def moved(at, k, count, back=False):
    if count & (count - 1):
        return lax.rem(at + (count - k if back else k), count)
    bit = 1
    while bit < count:
        if k & bit:
            at = at + bit * (1 - 2 * lax.rem(at // bit, 2))
        bit *= 2
    return at


def paired(experts):
    near, far = list(range(2, experts // 2)), list(range(experts // 2, experts))
    steps = [(0, 1)]
    for i in range(0, len(near), 2):
        steps += [(far[i],), (far[i + 1],), tuple(near[i:i + 2])]
    return steps + [(k,) for k in far[len(near):]]


def sequence(experts):
    near, far = list(range(2, experts // 2)), list(range(experts // 2, experts))
    both = [k for pair in zip(far, near) for k in pair]
    return both + far[len(near):]


def kernel(
    experts, shards, cap, tile,
    value_hbm, gatein_hbm, outer_hbm, conv_hbm, outw_hbm, tokens_hbm, gain_hbm, routes_hbm, rw_hbm,
    gate_hbm, up_hbm, down_hbm,
    both_ref,
    gate_w, up_w, down_w, value, gatein, outer, outw, tokens, conv_ref, gain_ref, routes_ref, rw_ref,
    routes_in, rw_in, normed, sent, weights, weights_in, slots, hidden, part, core_in, chip_in,
    back, back_in, cross_out, cross_in,
    prod, mixed, mpart, mcore, mx_in,
    w_sem, own_sem, out_s, out_r, xf_s, xf_r, df_s, df_r, dr_s, dr_r, xr_s, xr_r, bk_s, bk_r,
    h_s, h_r, md_s, md_r, mx_s, mx_r, rt_s, rt_r, pk_s, pk_r, cx_s, cx_r,
):
    high = shards // 2
    rows_own, features = tokens.shape
    slot_count = experts * cap
    me, mine = lax.axis_index("ep"), lax.axis_index("tp")
    low, top = lax.rem(mine, 2), mine // 2
    partner = (me, mine + 1 - 2 * low)
    across = (me, lax.rem(mine + high, shards))

    def to(k):
        return moved(me, k, experts)

    def source(k):
        return moved(me, k, experts, True)

    steps = paired(experts)
    stages = len(steps)
    stage = {k: j for j, ks in enumerate(steps) for k in ks}
    seat = {k: ks.index(k) * cap for ks in steps for k in ks}
    wide = [cap * len(ks) for ks in steps]
    half = [high * w for w in wide]
    base = [2 * sum(half[:j]) for j in range(stages)]
    part_base = [sum(half[:j]) for j in range(stages)]

    near = experts // 2
    first_near = (me // near) * near

    def rows_at(first, count):
        return pl.ds(pl.multiple_of(first, 16), count)

    def own_rows(j):
        return base[j] + low * half[j]

    def place(k):
        j = stage[k]
        return rows_at(own_rows(j) + top * wide[j] + seat[k], cap)

    def block(e):
        return pl.ds(pl.multiple_of(e * cap, 16), cap)

    def remote(src, dst, s, r, device):
        return pltpu.make_async_remote_copy(
            src_ref=src, dst_ref=dst, send_sem=s, recv_sem=r, device_id=device, device_id_type=MESH
        )

    barrier = pltpu.get_barrier_semaphore()
    for k in range(1, experts):
        pl.semaphore_signal(barrier, inc=1, device_id=(to(k), mine), device_id_type=MESH)
    for device in (partner, across):
        pl.semaphore_signal(barrier, inc=1, device_id=device, device_id_type=MESH)
    wanted = (
        (tokens_hbm, tokens), (gain_hbm, gain_ref), (routes_hbm, routes_ref),
        (value_hbm, value), (gatein_hbm, gatein), (outer_hbm, outer), (outw_hbm, outw),
        (conv_hbm, conv_ref), (rw_hbm, rw_ref),
        (gate_hbm, gate_w), (up_hbm, up_w), (down_hbm, down_w),
    )
    loads = [pltpu.make_async_copy(a, b, w_sem.at[i]) for i, (a, b) in enumerate(wanted)]
    for load in loads:
        load.start()

    out = [None] + [
        remote(
            sent.at[block(to(k))], slots.at[place(k)], out_s.at[k], out_r.at[k],
            (to(k), mine),
        )
        for k in range(1, experts)
    ]
    own_in = pltpu.make_async_copy(sent.at[block(me)], slots.at[place(0)], own_sem.at[0])
    groups = [(k,) for k in range(experts)]

    def crossing(i, ks):
        j = stage[ks[0]]
        here = slots.at[rows_at(own_rows(j) + top * wide[j] + seat[ks[0]], cap * len(ks))]
        return remote(
            here if ks[0] else sent.at[block(me)], here, xf_s.at[i], xf_r.at[i], across
        )

    x_out = {ks: crossing(i, ks) for i, ks in enumerate(groups)}

    def to_partner(j):
        here = slots.at[rows_at(own_rows(j), half[j])]
        return remote(here, here, df_s.at[j], df_r.at[j], partner)

    d_out = [to_partner(j) for j in range(stages)]
    d_back = [
        remote(
            part.at[rows_at(base[j] + (1 - low) * half[j], half[j])],
            core_in.at[rows_at(part_base[j], half[j])], dr_s.at[j], dr_r.at[j], partner,
        )
        for j in range(stages)
    ]
    def core_rows(k, of):
        j = stage[k]
        return core_in.at[rows_at(part_base[j] + of * wide[j] + seat[k], cap)]

    def chip_rows(k):
        return rows_at((k - near) * cap, cap)

    x_back = {
        k: remote(
            core_rows(k, 1 - top), chip_in.at[chip_rows(k)],
            xr_s.at[k - near], xr_r.at[k - near], across,
        )
        for k in range(near, experts)
    }
    home = {
        k: remote(
            chip_in.at[chip_rows(k)] if k >= near else core_rows(k, top), back.at[block(me)],
            bk_s.at[k], bk_r.at[k], (source(k), mine),
        )
        for k in range(1, experts)
    }
    home_in = {
        k: remote(
            core_rows(k, 1 - top), back_in.at[block(me - first_near)],
            pk_s.at[k], pk_r.at[k], (source(k), mine),
        )
        for k in range(1, near)
    }
    cross = remote(cross_out, cross_in, cx_s.at[0], cx_r.at[0], across)
    routing = [
        remote(routes_ref, routes_in, rt_s.at[0], rt_r.at[0], across),
        remote(rw_ref, rw_in, rt_s.at[1], rt_r.at[1], across),
    ]
    length = value.shape[0]
    halo = [
        remote(
            prod.at[pl.ds(length, HALO)], prod.at[pl.ds(0, HALO)], h_s.at[0], h_r.at[0],
            (lax.rem(me + 1, experts), mine),
        ),
        remote(
            prod.at[pl.ds(HALO, HALO)], prod.at[pl.ds(length + HALO, HALO)], h_s.at[1], h_r.at[1],
            (lax.rem(me + experts - 1, experts), mine),
        ),
    ]
    owned = length // shards

    def owner_rows(x, core):
        return pl.ds(pl.multiple_of((2 * x + core) * owned, 16), owned)

    m_core = [
        remote(
            mpart.at[owner_rows(x, 1 - low)], mcore.at[x], md_s.at[x], md_r.at[x], partner
        )
        for x in range(high)
    ]
    unit = owned // sum(PIECES)
    pieces = [pl.ds(sum(PIECES[:i]) * unit, count * unit) for i, count in enumerate(PIECES)]
    m_across = [
        remote(mcore.at[1 - top, at], mx_in.at[at], mx_s.at[i], mx_r.at[i], across)
        for i, at in enumerate(pieces)
    ]

    for load in loads[:3]:
        load.wait()
    gain = gain_ref[...].astype(F32).reshape(1, features)

    def norm(i, carry):
        at = pl.ds(pl.multiple_of(i * 32, 32), 32)
        x = tokens[at, :].astype(F32)
        scale = lax.rsqrt(jnp.mean(x * x, axis=-1, keepdims=True) + 1e-06)
        normed[at, :] = (x * scale * gain).astype(BF16)
        return carry

    lax.fori_loop(0, rows_own // 32, norm, 0)
    lines = 16 * (-(-experts // 16))
    expert_ids = lax.broadcasted_iota(jnp.int32, (lines, rows_own), 0)
    before = (
        lax.broadcasted_iota(jnp.int32, (rows_own, rows_own), 0)
        < lax.broadcasted_iota(jnp.int32, (rows_own, rows_own), 1)
    ).astype(F32).astype(BF16)

    def slots_of(routes, start, count):
        chosen = [(expert_ids == routes[i:i + 1, :]).astype(F32) for i in range(2)]
        named = (chosen[0] + chosen[1]).astype(BF16)
        rank = jnp.dot(named, before, preferred_element_type=F32)
        ids = (lax.broadcasted_iota(jnp.int32, (count, rows_own), 0) + start).astype(F32)

        def at_slot(i):
            position = jnp.sum(chosen[i] * rank, axis=0, keepdims=True)
            return (ids == routes[i:i + 1, :].astype(F32) * cap + position).astype(F32)

        return at_slot(0), at_slot(1)

    def weigh(ref, at_first, at_second, rw):
        mix = at_first * rw[0:1, :] + at_second * rw[1:2, :]
        leading = mix.astype(BF16).astype(F32)
        ref[pl.ds(0, rows_own), :] = leading.T.astype(BF16)
        ref[pl.ds(rows_own, rows_own), :] = (mix - leading).T.astype(BF16)

    at_first, at_second = slots_of(routes_ref[...], 0, slot_count)
    placement = (at_first + at_second).astype(BF16)

    def gather(i, carry):
        at = pl.ds(pl.multiple_of(i * tile, tile), tile)
        sent[:, at] = jnp.dot(
            placement, normed[:, at], preferred_element_type=F32
        ).astype(BF16)
        return carry

    lax.fori_loop(0, features // tile, gather, 0)
    loads[3].wait()
    loads[4].wait()

    def multiply(first, count):
        at = pl.ds(first, count)
        prod[pl.ds(HALO + first, count), :] = (
            value[at, :].astype(F32) * gatein[at, :].astype(F32)
        ).astype(BF16)

    multiply(0, HALO)
    multiply(length - HALO, HALO)
    pl.semaphore_wait(barrier, experts + 1)
    x_out[0,].start()
    loads[8].wait()
    for copy in routing:
        copy.start()
    for copy in halo:
        copy.start()
    for k in sequence(experts) + [1]:
        out[k].start()
    own_in.start()

    multiply(HALO, length - 2 * HALO)
    for load in loads[5:8]:
        load.wait()
    for copy in halo:
        copy.wait()
    keep_first = jnp.where(me == 0, 0.0, 1.0)
    keep_last = jnp.where(me == experts - 1, 0.0, 1.0)
    prod[pl.ds(0, HALO), :] = (prod[pl.ds(0, HALO), :].astype(F32) * keep_first).astype(BF16)
    last = pl.ds(length + HALO, HALO)
    prod[last, :] = (prod[last, :].astype(F32) * keep_last).astype(BF16)
    taps = conv_ref[...].astype(F32)

    def mix_rows(x, core):
        start = pl.multiple_of((2 * x + core) * owned, 16)
        span = owned + 2 * HALO
        p = prod[pl.ds(start, span), :].astype(F32)
        convolved = (
            pltpu.roll(p, 1, 0) * taps[0:1] + p * taps[1:2] + pltpu.roll(p, span - 1, 0) * taps[2:3]
        )[HALO:HALO + owned]
        mixed[...] = (outer[pl.ds(start, owned), :].astype(F32) * convolved).astype(BF16)

        def step(i, carry):
            at = pl.ds(pl.multiple_of(i * tile, tile), tile)
            mpart[pl.ds(start, owned), at] = jnp.dot(
                mixed[...], outw[:, at], preferred_element_type=F32
            ).astype(BF16)
            return carry

        lax.fori_loop(0, features // tile, step, 0)

    for x in range(high):
        mix_rows(x, 1 - low)
        m_core[x].start()

    weigh(weights, at_first, at_second, rw_ref[...])
    own_in.wait()

    def arrive(*ks):
        for k in ks:
            out[k].wait_recv()
        x_out[ks].start()

    arrive(1)
    for x in range(high):
        mix_rows(x, low)
    for x in range(high):
        m_core[x].wait_recv()

    theirs = pl.multiple_of((2 * (1 - top) + low) * owned, 16)

    def sum_across(i, carry):
        at = pl.ds(pl.multiple_of(i * 16, 16), 16)
        mcore[1 - top, at] = (
            mcore[1 - top, at].astype(F32)
            + mpart[pl.ds(pl.multiple_of(theirs + i * 16, 16), 16), :].astype(F32)
        ).astype(BF16)
        return carry

    lax.fori_loop(0, owned // 16, sum_across, 0)
    m_across[0].start()

    def spread(j):
        for ks in groups:
            if stage[ks[0]] == j:
                x_out[ks].wait_recv()
        d_out[j].start()

    def activate(j, hooks):
        d_out[j].wait_recv()

        def step(i, carry):
            for at_step, hook in hooks:
                @pl.when(i == at_step)
                def _():
                    hook()

            at = pl.ds(pl.multiple_of(i * tile, tile), tile)
            x = slots[pl.ds(base[j], 2 * half[j]), :]
            g = jnp.dot(x, gate_w[:, at], preferred_element_type=F32)
            u = jnp.dot(x, up_w[:, at], preferred_element_type=F32)
            hidden[pl.ds(0, 2 * half[j]), at] = (g / (1.0 + jnp.exp(-g)) * u).astype(BF16)
            return carry

        lax.fori_loop(0, gate_w.shape[1] // tile, step, 0)

    def project(j):
        def step(i, carry):
            at = pl.ds(pl.multiple_of(i * 2 * tile, 2 * tile), 2 * tile)
            part[pl.ds(base[j], 2 * half[j]), at] = jnp.dot(
                hidden[pl.ds(0, 2 * half[j]), :], down_w[:, at], preferred_element_type=F32
            ).astype(BF16)
            return carry

        lax.fori_loop(0, down_w.shape[1] // (2 * tile), step, 0)
        d_back[j].start()

    def pair_sum(k, of, ref, start):
        j = stage[k]

        def step(i, carry):
            first = of * wide[j] + seat[k] + i * 16
            ref[rows_at(start + i * 16, 16), :] = (
                part[rows_at(own_rows(j) + first, 16), :].astype(F32)
                + core_in[rows_at(part_base[j] + first, 16), :].astype(F32)
            ).astype(BF16)
            return carry

        lax.fori_loop(0, cap // 16, step, 0)

    def pair_up(j):
        d_back[j].wait_recv()
        for k in steps[j]:
            at = part_base[j] + seat[k]
            if k == 0:
                pair_sum(k, top, back, me * cap)
                pair_sum(k, 1 - top, back_in, (me - first_near) * cap)
                continue
            pair_sum(k, 1 - top, core_in, at + (1 - top) * wide[j])
            if k >= near:
                x_back[k].start()
                continue
            home_in[k].start()
            pair_sum(k, top, core_in, at + top * wide[j])
            home[k].start()

    def finish(k):
        j = stage[k]
        x_back[k].wait_recv()

        def step(i, carry):
            here = rows_at((k - near) * cap + i * 16, 16)
            first = top * wide[j] + seat[k] + i * 16
            chip_in[here, :] = (
                part[rows_at(own_rows(j) + first, 16), :].astype(F32)
                + core_in[rows_at(part_base[j] + first, 16), :].astype(F32)
                + chip_in[here, :].astype(F32)
            ).astype(BF16)
            return carry

        lax.fori_loop(0, cap // 16, step, 0)
        home[k].start()

    def finish_all(j):
        for k in steps[j]:
            if k >= near:
                finish(k)

    waiting = sequence(experts)

    def arrive_to(j):
        while any(k in waiting for ks in steps[:j + 1] for k in ks):
            arrive(waiting.pop(0))

    for k in range(2):
        arrive(waiting.pop(0))
    spread(0)
    for copy in routing:
        copy.wait_recv()
    weigh(
        weights_in, *slots_of(routes_in[...], first_near * cap, near * cap), rw_in[...]
    )
    for i in range(stages):
        hooks = []
        if i == 0:
            hooks.append((2, functools.partial(spread, 1)))
            loads[9].wait()
            loads[10].wait()
        else:
            hooks.append((1, functools.partial(arrive_to, i + 2)))
            hooks.append((2, functools.partial(pair_up, i - 1)))
        activate(i, hooks)
        if i == 0:
            arrive_to(2)
            loads[11].wait()
        elif i + 1 < stages:
            spread(i + 1)
        if i == 3:
            finish_all(1)
        project(i)
        if i > 3:
            finish_all(i - 2)
    pair_up(stages - 1)
    for copy in m_across[1:]:
        copy.start()
    finish_all(stages - 2)
    finish_all(stages - 1)
    for k in range(1, near):
        home_in[k].wait_recv()

    def combine_in(i, carry):
        at = pl.ds(pl.multiple_of(i * tile, tile), tile)
        both = jnp.dot(weights_in[...], back_in[:, at], preferred_element_type=F32)
        cross_out[:, at] = (both[:rows_own] + both[rows_own:]).astype(BF16)
        return carry

    lax.fori_loop(0, features // tile, combine_in, 0)
    cross.start()

    for copy in m_across:
        copy.wait_recv()
    mine_rows = pl.multiple_of(mine * owned, 16)

    def sum_own(i, carry):
        at = pl.ds(pl.multiple_of(i * 16, 16), 16)
        both_ref[at, :] = (
            mpart[pl.ds(pl.multiple_of(mine_rows + i * 16, 16), 16), :].astype(F32)
            + mcore[top, at].astype(F32)
            + mx_in[at, :].astype(F32)
        ).astype(BF16)
        return carry

    lax.fori_loop(0, owned // 16, sum_own, 0)
    for k in range(1, experts):
        home[k].wait()
    cross.wait()

    def combine(i, carry):
        at = pl.ds(pl.multiple_of(i * tile, tile), tile)
        both = jnp.dot(weights[...], back[:, at], preferred_element_type=F32)
        both_ref[pl.ds(owned, rows_own), at] = (
            both[:rows_own] + both[rows_own:] + cross_in[:, at].astype(F32)
        ).astype(BF16)
        return carry

    lax.fori_loop(0, features // tile, combine, 0)
    for k in range(1, experts):
        out[k].wait_send()
    for copy in list(x_out.values()) + list(x_back.values()) + list(home_in.values()) + routing:
        copy.wait_send()
    for j in range(stages):
        d_out[j].wait_send()
        d_back[j].wait_send()
    for copy in m_core + m_across:
        copy.wait_send()


def body(
    value_in, gate_in, outer_gate, conv_weight, out_weight, moe_tokens, norm_gain, routes,
    route_weight, expert_gate, expert_up, expert_down,
):
    row_total, top_count = routes.shape
    features = moe_tokens.shape[1]
    length, channels = value_in.shape
    local_units = expert_gate.shape[2]
    experts, shards = lax.axis_size("ep"), lax.axis_size("tp")
    capacity = 3 * top_count * row_total // (2 * experts)
    capacity = -(-capacity // 16) * 16
    slots = experts * capacity
    steps = paired(experts)
    stages, total = len(steps), slots * shards
    owned = length // shards
    dma = pltpu.SemaphoreType.DMA
    vmem, hbm = pl.BlockSpec(memory_space=pltpu.VMEM), pl.BlockSpec(memory_space=pl.ANY)
    both = pl.pallas_call(
        functools.partial(kernel, experts, shards, capacity, 512),
        out_shape=jax.ShapeDtypeStruct((owned + row_total, features), BF16),
        in_specs=[hbm] * 12,
        out_specs=vmem,
        scratch_shapes=[
            pltpu.VMEM((features, local_units), BF16),
            pltpu.VMEM((features, local_units), BF16),
            pltpu.VMEM((local_units, features), BF16),
            pltpu.VMEM((length, channels), BF16),
            pltpu.VMEM((length, channels), BF16),
            pltpu.VMEM((length, channels), BF16),
            pltpu.VMEM((channels, features), BF16),
            pltpu.VMEM((row_total, features), BF16),
            pltpu.VMEM(conv_weight.shape, BF16),
            pltpu.VMEM(norm_gain.shape, BF16),
            pltpu.VMEM((top_count, row_total), jnp.int32),
            pltpu.VMEM((top_count, row_total), F32),
            pltpu.VMEM((top_count, row_total), jnp.int32),
            pltpu.VMEM((top_count, row_total), F32),
            pltpu.VMEM((row_total, features), BF16),
            pltpu.VMEM((slots, features), BF16),
            pltpu.VMEM((2 * row_total, slots), BF16),
            pltpu.VMEM((2 * row_total, slots // 2), BF16),
            pltpu.VMEM((total, features), BF16),
            pltpu.VMEM((2 * shards * capacity, local_units), BF16),
            pltpu.VMEM((total, features), BF16),
            pltpu.VMEM((total // 2, features), BF16),
            pltpu.VMEM((slots // 2, features), BF16),
            pltpu.VMEM((slots, features), BF16),
            pltpu.VMEM((slots // 2, features), BF16),
            pltpu.VMEM((row_total, features), BF16),
            pltpu.VMEM((row_total, features), BF16),
            pltpu.VMEM((length + 2 * HALO, channels), BF16),
            pltpu.VMEM((owned, channels), BF16),
            pltpu.VMEM((length, features), BF16),
            pltpu.VMEM((shards // 2, owned, features), BF16),
            pltpu.VMEM((owned, features), BF16),
            dma((12,)),
            dma((1,)),
        ]
        + [dma((experts,))] * 4
        + [dma((stages,))] * 4
        + [dma((experts,))] * 4
        + [dma((2,))] * 4
        + [dma((len(PIECES),))] * 2
        + [dma((2,))] * 2
        + [dma((experts // 2,))] * 2
        + [dma((1,))] * 2,
        compiler_params=pltpu.CompilerParams(
            collective_id=0, has_side_effects=True, vmem_limit_bytes=67043328
        ),
        cost_estimate=pl.CostEstimate(
            flops=6 * total * features * local_units,
            bytes_accessed=6 * features * local_units,
            transcendentals=total * local_units,
        ),
    )(
        value_in, gate_in, outer_gate, conv_weight, out_weight, moe_tokens,
        norm_gain, routes.T, route_weight.T,
        expert_gate[0], expert_up[0], expert_down[0],
    )
    return both[:owned], both[owned:]


def solution(mesh):
    placed = (
        P("ep", "tp"),
        P("ep", "tp"),
        P("ep", "tp"),
        P(None, "tp"),
        P("tp", None),
        P(("ep", "tp"), None),
        P(),
        P(("ep", "tp"), None),
        P(("ep", "tp"), None),
        P("ep", None, "tp"),
        P("ep", None, "tp"),
        P("ep", "tp", None),
    )
    return jax.shard_map(
        body,
        mesh=mesh,
        in_specs=placed,
        out_specs=(P(("ep", "tp"), None), P(("ep", "tp"), None)),
        check_vma=False,
    )
```
